512 devices in a mesh: grp: 2 (over y), fs: 32 (over z), tp: 8 (over x, core).
Axes of the slice: x: 4, y: 2, z: 32, core: 2. Of those that a mesh axis runs over, the one named last changes fastest.
The devices are a block of a 4x8x32 slice.
Arguments:
- tokens: bfloat16 [65536, 2048], P(('grp', 'fs')), parts along dimension 0, may hold values from -6 to 6
- mixer_gain: float32 [2048], replicated, may hold values from 0.1 to 1.9
- outer_weight: float32 [2048, 2048], P('fs', 'tp'), may hold values from -0.125 to 0.125
- inner_weight: float32 [2048, 2048], P('fs', 'tp'), may hold values from -0.125 to 0.125
- value_weight: float32 [2048, 2048], P('fs', 'tp'), may hold values from -0.125 to 0.125
- filter_taps: float32 [3, 2048], P(None, 'tp'), may hold values from -3.5 to 3.5
- mixer_weight: float32 [2048, 2048], P('tp', 'fs'), may hold values from -0.125 to 0.125
- outer_scale: float32 [8, 256], P('tp', 'fs'), may hold values from 0.5 to 2
- inner_scale: float32 [8, 256], P('tp', 'fs'), may hold values from 0.5 to 2
- value_scale: float32 [8, 256], P('tp', 'fs'), may hold values from 0.5 to 2
- mixer_scale: float32 [1, 2048], P(None, 'fs'), may hold values from 0.5 to 2
Outputs:
- layer_out: bfloat16 [65536, 2048], P(('grp', 'fs', 'tp')), parts along dimension 0
The draws below stay inside these ranges and needn't reach their ends.
There are 2 independent parts, one for each index of `grp`. The reference program is written for one: setup_inputs(seed, part) draws one part's arguments, and reference() takes and returns one part's arrays. A program takes and returns all parts, laid end to end along the dimension named above; an argument that names none is the same for every part. Nothing has to cross between parts.
All inputs are finite; a program needn't handle non-finite values.
Results may differ from the reference program's by a relative error of at most 0.014.
Values may be sent and summed in bfloat16 or wider, within the bound.
No kernel may reach another device: no remote copies, remote signals or barrier semaphores. Data moves between devices by JAX's collectives and lax.ppermute only.
A program may use at most 64 MiB of HBM per device.

```python
import math
import jax
import jax.numpy as jnp
from jax import lax

D = 2048
DC = 2048
SEQ_LEN = 1024
TOKENS = 32768
N_FS = 32
N_TP = 8


def levels(key, dims, shards, smallest, top_value):
    factor_of = 1.0
    for axis_at, blocks in shards:
        heights = jax.random.uniform(jax.random.fold_in(jax.random.fold_in(key, 6), axis_at), (blocks,), jnp.float32, smallest / len(shards), top_value / len(shards))
        factor_of = factor_of * jnp.repeat(jnp.exp(heights), dims[axis_at] // blocks).reshape((-1,) + (1,) * (len(dims) - 1 - axis_at))
    return factor_of


def centred(stream_key, dims, scale, reach, cuts=(), held_as=jnp.bfloat16):
    drawn = scale * jax.random.normal(stream_key, dims, jnp.float32)
    if cuts:
        drawn = drawn * levels(stream_key, dims, cuts, -0.22, 0.18)
    return jnp.clip(drawn, -reach, reach).astype(held_as)


def setup_inputs(seed: int = 0, part: int = 0) -> dict:
    streams_of = jax.random.split(jax.random.key(seed), 12)
    own_keys = jax.random.split(jax.random.fold_in(streams_of[11], part), 12)
    tokens = centred(own_keys[0], (TOKENS, D), 1.0, 6.0, ((0, 32),))
    mixer_gain = jnp.clip(1.0 + 0.18 * jax.random.normal(streams_of[1], (D,), jnp.float32), 0.1, 1.9)
    outer_weight = centred(streams_of[2], (D, DC), D ** -0.5, 0.125, ((0, 32), (1, 8)), jnp.float32)
    inner_weight = centred(streams_of[3], (D, DC), D ** -0.5, 0.125, ((0, 32), (1, 8)), jnp.float32)
    value_weight = centred(streams_of[4], (D, DC), D ** -0.5, 0.125, ((0, 32), (1, 8)), jnp.float32)
    filter_taps = centred(streams_of[5], (3, DC), 3 ** -0.5, 3.5, ((1, 8),), jnp.float32)
    mixer_weight = centred(streams_of[6], (DC, D), DC ** -0.5, 0.125, ((0, 8), (1, 32)), jnp.float32)
    outer_scale = jnp.clip(jnp.exp(math.log(2.0) - 1.3862944 * jax.random.uniform(streams_of[7], (N_TP, DC // N_TP), jnp.float32) ** levels(streams_of[7], (N_TP, DC // N_TP), ((0, 8), (1, 32)), -0.2, 0.2)), 0.5, 2.0)
    inner_scale = jnp.clip(jnp.exp(math.log(2.0) - 1.3862944 * jax.random.uniform(streams_of[8], (N_TP, DC // N_TP), jnp.float32) ** levels(streams_of[8], (N_TP, DC // N_TP), ((0, 8), (1, 32)), -0.2, 0.2)), 0.5, 2.0)
    value_scale = jnp.clip(jnp.exp(math.log(2.0) - 1.3862944 * jax.random.uniform(streams_of[9], (N_TP, DC // N_TP), jnp.float32) ** levels(streams_of[9], (N_TP, DC // N_TP), ((0, 8), (1, 32)), -0.2, 0.2)), 0.5, 2.0)
    mixer_scale = jnp.clip(jnp.exp(math.log(2.0) - 1.3862944 * jax.random.uniform(streams_of[10], (1, D), jnp.float32) ** levels(streams_of[10], (1, D), ((1, 32),), -0.2, 0.2)), 0.5, 2.0)
    return dict(tokens=tokens, mixer_gain=mixer_gain, outer_weight=outer_weight, inner_weight=inner_weight, value_weight=value_weight, filter_taps=filter_taps, mixer_weight=mixer_weight, outer_scale=outer_scale, inner_scale=inner_scale, value_scale=value_scale, mixer_scale=mixer_scale)


EPS = 1e-06

def normed(rows, gain):
    values = rows.astype(jnp.float32)
    inverse = lax.rsqrt(lax.optimization_barrier(jnp.mean(values * values, axis=-1, keepdims=True)) + EPS)
    return (values * inverse * gain).astype(jnp.bfloat16)

def project(left, weight, scale):
    return jnp.dot(left, weight.astype(jnp.bfloat16), preferred_element_type=jnp.float32) * scale.reshape(-1)

def rounded(values):
    return lax.optimization_barrier(values.astype(jnp.bfloat16)).astype(jnp.float32)

def summed_blocks(hidden, weight, scale):
    width = hidden.shape[1] // N_TP
    total = jnp.zeros((hidden.shape[0], weight.shape[1]), jnp.float32)
    for index in range(N_TP):
        part = project(hidden[:, index * width:(index + 1) * width], weight[index * width:(index + 1) * width], scale)
        total = total + rounded(part)
    return total

def reference(tokens, mixer_gain, outer_weight, inner_weight, value_weight, filter_taps, mixer_weight, outer_scale, inner_scale, value_scale, mixer_scale):
    normal_rows = normed(tokens, mixer_gain)
    outer = rounded(project(normal_rows, outer_weight, outer_scale))
    inner = rounded(project(normal_rows, inner_weight, inner_scale))
    value = rounded(project(normal_rows, value_weight, value_scale))
    product = (inner * value).reshape(N_FS, SEQ_LEN, DC)
    padded = jnp.pad(product, ((0, 0), (2, 0), (0, 0)))
    filtered = filter_taps[0] * padded[:, 0:SEQ_LEN] + filter_taps[1] * padded[:, 1:SEQ_LEN + 1] + filter_taps[2] * padded[:, 2:]
    gated = (outer * filtered.reshape(TOKENS, DC)).astype(jnp.bfloat16)
    return summed_blocks(gated, mixer_weight, mixer_scale).astype(jnp.bfloat16)
```

```python
import jax
import jax.numpy as jnp
from jax import lax
from jax.sharding import PartitionSpec as P

EPS = 1e-06
LIFT = 2.0**18
LOW = 2.0**12
LANES = 128


def normed(rows, gain):
    values = rows.astype(jnp.float32)
    inverse = lax.rsqrt(jnp.mean(values * values, axis=-1, keepdims=True) + EPS)
    return (values * inverse * gain).astype(jnp.bfloat16)


def rounded(values):
    return lax.optimization_barrier(values.astype(jnp.bfloat16)).astype(jnp.float32)


def lifted(weight):
    return (weight.astype(jnp.bfloat16).astype(jnp.float32) * LIFT).astype(jnp.float16)


def lane_blocks(array):
    return [array[:, at : at + LANES] for at in range(0, array.shape[1], LANES)]


def scale_rows(scales):
    flat = jnp.concatenate([s.reshape(-1) for s in scales])
    flat = jnp.pad(flat, (0, LANES - flat.size))
    high = flat.astype(jnp.float16)
    low = ((flat - high.astype(jnp.float32)) * LOW).astype(jnp.float16)
    return jnp.pad(jnp.stack([high, low]), ((0, 6), (0, 0)))


def gathered(weights, scales):
    rows = weights[0].shape[0]
    blocks = [b for w in weights for b in lane_blocks(lifted(w))]
    packed = jnp.concatenate(blocks + [scale_rows(scales)], axis=0)
    pieces = lax.all_gather(packed, "fs")
    count = pieces.shape[0]

    def block(at):
        return pieces[:, at * rows : (at + 1) * rows].reshape(count * rows, LANES)

    full, at = [], 0
    for w in weights:
        width = w.shape[1] // LANES
        both = jnp.concatenate([block(at + k) for k in range(width)], axis=1)
        full.append(both.astype(jnp.float32).astype(jnp.bfloat16))
        at += width
    top = pieces[:, at * rows].astype(jnp.float32) + pieces[:, at * rows + 1].astype(
        jnp.float32
    ) * (1.0 / LOW)
    columns, start = [], 0
    for s in scales:
        columns.append(top[:, start : start + s.size].reshape(-1) * (1.0 / LIFT))
        start += s.size
    return full, columns


def summed_rows(left, weight, scale):
    count = lax.axis_size("tp")
    chips = count // 2
    me = lax.axis_index("tp")
    chip, core = me // 2, me % 2
    rows = left.shape[0] // count
    width = left.shape[1]
    grid = left.reshape(chips, 2, rows, width)

    def mine(which):
        picked = lax.dynamic_slice_in_dim(grid, which, 1, 1).reshape(chips, rows, width)
        twice = jnp.concatenate([picked, picked], axis=0)
        return lax.dynamic_slice_in_dim(twice, chip, chips, 0).reshape(chips * rows, width)

    def part(these):
        return (
            lax.dot_general(
                these, weight, (((1,), (1,)), ((), ())), preferred_element_type=jnp.float32
            )
            * scale
        )

    swap = [(i, i ^ 1) for i in range(count)]
    theirs = lax.ppermute(part(mine(1 - core)).astype(jnp.bfloat16), "tp", swap)
    pair = part(mine(core)).astype(jnp.bfloat16).astype(jnp.float32) + theirs.astype(jnp.float32)
    total = pair[:rows]
    for step in range(1, chips):
        move = [(i, (i + 2 * step) % count) for i in range(count)]
        sent = pair[step * rows : (step + 1) * rows].astype(jnp.bfloat16)
        total = total + lax.ppermute(sent, "tp", move).astype(jnp.float32)
    return total.astype(jnp.bfloat16)


def per_device(
    tokens,
    mixer_gain,
    outer_weight,
    inner_weight,
    value_weight,
    filter_taps,
    mixer_weight,
    outer_scale,
    inner_scale,
    value_scale,
    mixer_scale,
):
    seq_rows = tokens.shape[0]
    full, columns = gathered(
        (outer_weight, inner_weight, value_weight, mixer_weight.T),
        (outer_scale, inner_scale, value_scale, mixer_scale),
    )
    normal_rows = normed(tokens, mixer_gain)
    outer, inner, value = [
        rounded(jnp.dot(normal_rows, w, preferred_element_type=jnp.float32) * c)
        for w, c in zip(full[:3], columns[:3])
    ]
    padded = jnp.pad(inner * value, ((2, 0), (0, 0)))
    filtered = (
        filter_taps[0] * padded[0:seq_rows]
        + filter_taps[1] * padded[1 : seq_rows + 1]
        + filter_taps[2] * padded[2:]
    )
    gated = (outer * filtered).astype(jnp.bfloat16)
    return summed_rows(gated, full[3], columns[3])


def solution(mesh):
    in_specs = (
        P(("grp", "fs"), None),
        P(),
        P("fs", "tp"),
        P("fs", "tp"),
        P("fs", "tp"),
        P(None, "tp"),
        P("tp", "fs"),
        P("tp", "fs"),
        P("tp", "fs"),
        P("tp", "fs"),
        P(None, "fs"),
    )
    out_specs = P(("grp", "fs", "tp"), None)
    return jax.shard_map(
        per_device, mesh=mesh, in_specs=in_specs, out_specs=out_specs, check_vma=False
    )
```

```python
import jax
import jax.numpy as jnp
from jax import lax
from jax.experimental import pallas as pl
from jax.experimental.pallas import tpu as pltpu
from jax.sharding import PartitionSpec as P

EPS = 1e-06
LIFT = 2.0**18
LOW = 2.0**12
LANES = 128
ROWS = 256
VMEM_BYTES = 28 * 2**20


def pack_kernel(*refs):
    *arrays, out = refs
    weights, scales = arrays[:4], arrays[4:]
    at = 0
    for w in weights:
        rows, width = w.shape
        for k in range(0, width, LANES):
            block = w[:, k : k + LANES].astype(jnp.bfloat16).astype(jnp.float32)
            out[at : at + rows, :] = block * LIFT
            at += rows
    out[at:, :] = jnp.zeros((out.shape[0] - at, LANES), jnp.float32)
    start = 0
    for s in scales:
        value, stop = s[...], start + s.shape[1]
        high = value.astype(jnp.bfloat16).astype(jnp.float32)
        rest = (value - high) * LOW
        middle = rest.astype(jnp.bfloat16).astype(jnp.float32)
        for k, term in enumerate((high, middle, rest - middle)):
            out[at + k : at + k + 1, start:stop] = term
        start = stop


def gathered(weights, scales):
    rows = weights[0].shape[0]
    total = sum(w.shape[1] for w in weights) // LANES * rows + 8
    packed = pl.pallas_call(
        pack_kernel,
        out_shape=jax.ShapeDtypeStruct((total, LANES), jnp.float32),
        compiler_params=pltpu.CompilerParams(vmem_limit_bytes=4 * 2**20),
    )(*weights, *scales)
    pieces = lax.all_gather(packed.astype(jnp.float16), "fs")
    blocks = pieces.shape[1] // rows
    terms = [pieces[:, blocks * rows + k].astype(jnp.float32) for k in range(3)]
    top = terms[0] + (terms[1] + terms[2]) * (1.0 / LOW)
    columns, start = [], 0
    for s in scales:
        columns.append(top[:, start : start + s.size].reshape(-1) * (1.0 / LIFT))
        start += s.size
    pieces = lax.optimization_barrier(pieces.astype(jnp.float32).astype(jnp.bfloat16))
    pieces = pltpu.with_memory_space_constraint(pieces, pltpu.VMEM)
    return pieces, (jnp.concatenate(columns[:-1]), columns[-1])


def summed_rows(left, weight, scale):
    count = lax.axis_size("tp")
    chips = count // 2
    core = lax.axis_index("tp") % 2
    rows = left.shape[0] // count
    grid = left.reshape(chips, 2, rows, left.shape[1])

    def part(which):
        these = lax.dynamic_slice_in_dim(grid, which, 1, 1).reshape(chips * rows, -1)
        return (
            lax.dot_general(
                these, weight, (((1,), (1,)), ((), ())), preferred_element_type=jnp.float32
            )
            * scale
        ).astype(jnp.bfloat16)

    swap = [(i, i ^ 1) for i in range(count)]
    theirs = lax.ppermute(part(1 - core), "tp", swap)
    pair = (part(core).astype(jnp.float32) + theirs.astype(jnp.float32)).astype(jnp.bfloat16)
    same_core = [list(range(which, count, 2)) for which in range(2)]
    parts = lax.all_to_all(
        pair.reshape(chips, rows, -1), "tp", 0, 0, axis_index_groups=same_core
    )
    total = parts[0].astype(jnp.float32)
    for k in range(1, chips):
        total = total + parts[k].astype(jnp.float32)
    return total.astype(jnp.bfloat16)


def gate_kernel(tokens, gain, pieces, columns, taps, out, mixer, weight, carry):
    @pl.when(pl.program_id(0) == 0)
    def _():
        carry[...] = jnp.zeros_like(carry)
        depth = weight.shape[0]
        rows = depth // pieces.shape[0]
        inputs = weight.shape[1] // LANES
        for k in range(inputs + mixer.shape[1] // LANES):
            full = pieces[:, k * rows : (k + 1) * rows, :]
            to, at = (weight, k) if k < inputs else (mixer, k - inputs)
            to[:, at * LANES : (at + 1) * LANES] = full.reshape(depth, LANES)

    values = tokens[...].astype(jnp.float32)
    inverse = lax.rsqrt(jnp.mean(values * values, axis=-1, keepdims=True) + EPS)
    normal = (values * inverse * gain[...]).astype(jnp.bfloat16)
    width = out.shape[1]

    def projected(at):
        cols = slice(at * width, (at + 1) * width)
        total = jnp.dot(normal, weight[:, cols], preferred_element_type=jnp.float32)
        return (total * columns[:, cols]).astype(jnp.bfloat16).astype(jnp.float32)

    product = projected(1) * projected(2)
    last = carry[...]
    carry[...] = product[-8:]
    row = lax.broadcasted_iota(jnp.int32, (8, width), 0)

    def shifted(by):
        moved = pltpu.roll(product, by, 0)
        head = jnp.where(row < by, pltpu.roll(last, by, 0), moved[:8])
        return jnp.concatenate([head, moved[8:]], axis=0)

    filtered = taps[0:1] * shifted(2) + taps[1:2] * shifted(1) + taps[2:3] * product
    out[...] = (projected(0) * filtered).astype(jnp.bfloat16)


def gated_rows(tokens, gain, pieces, columns, taps):
    rows, depth = tokens.shape
    width = taps.shape[1]
    whole = pl.BlockSpec(memory_space=pltpu.VMEM)
    return pl.pallas_call(
        gate_kernel,
        grid=(rows // ROWS,),
        in_specs=[pl.BlockSpec((ROWS, depth), lambda i: (i, 0)), whole, whole, whole, whole],
        out_specs=[pl.BlockSpec((ROWS, width), lambda i: (i, 0)), whole],
        out_shape=[
            jax.ShapeDtypeStruct((rows, width), jnp.bfloat16),
            jax.ShapeDtypeStruct((depth, width), jnp.bfloat16),
        ],
        scratch_shapes=[
            pltpu.VMEM((depth, 3 * width), jnp.bfloat16),
            pltpu.VMEM((8, width), jnp.float32),
        ],
        compiler_params=pltpu.CompilerParams(
            dimension_semantics=("arbitrary",), vmem_limit_bytes=VMEM_BYTES
        ),
    )(pltpu.with_memory_space_constraint(tokens, pltpu.HBM), gain.reshape(1, -1), pieces, columns.reshape(1, -1), taps)


def per_device(
    tokens,
    mixer_gain,
    outer_weight,
    inner_weight,
    value_weight,
    filter_taps,
    mixer_weight,
    outer_scale,
    inner_scale,
    value_scale,
    mixer_scale,
):
    pieces, columns = gathered(
        (outer_weight, inner_weight, value_weight, mixer_weight.T),
        (outer_scale, inner_scale, value_scale, mixer_scale),
    )
    gated, mixer_full = gated_rows(tokens, mixer_gain, pieces, columns[0], filter_taps)
    return summed_rows(gated, mixer_full, columns[1])


def solution(mesh):
    in_specs = (
        P(("grp", "fs"), None),
        P(),
        P("fs", "tp"),
        P("fs", "tp"),
        P("fs", "tp"),
        P(None, "tp"),
        P("tp", "fs"),
        P("tp", "fs"),
        P("tp", "fs"),
        P("tp", "fs"),
        P(None, "fs"),
    )
    out_specs = P(("grp", "fs", "tp"), None)
    return jax.shard_map(
        per_device, mesh=mesh, in_specs=in_specs, out_specs=out_specs, check_vma=False
    )
```

```python
import jax
import jax.numpy as jnp
from jax import lax
from jax.experimental import pallas as pl
from jax.experimental.pallas import tpu as pltpu
from jax.sharding import PartitionSpec as P


EPS = 1e-06
LIFT = 2.0**18
LOW = 2.0**12
LANES = 128
PARTS = 2
ROWS = 256
VMEM_BYTES = 28 * 2**20


def pack_kernel(*refs):
    *arrays, out = refs
    weights, scales = arrays[:4], arrays[4:]
    at = 0
    for w in weights:
        rows, width = w.shape
        for k in range(0, width, LANES):
            block = w[:, k : k + LANES].astype(jnp.bfloat16).astype(jnp.float32)
            out[at : at + rows, :] = block * LIFT
            at += rows
    out[at:, :] = jnp.zeros((out.shape[0] - at, LANES), jnp.float32)
    start = 0
    for s in scales:
        value, stop = s[...], start + s.shape[1]
        high = value.astype(jnp.bfloat16).astype(jnp.float32)
        rest = (value - high) * LOW
        middle = rest.astype(jnp.bfloat16).astype(jnp.float32)
        for k, term in enumerate((high, middle, rest - middle)):
            out[at + k : at + k + 1, start:stop] = term
        start = stop


def gathered(weights, scales):
    rows = weights[0].shape[0]
    total = sum(w.shape[1] for w in weights) // LANES * rows + 8
    packed = pl.pallas_call(
        pack_kernel,
        out_shape=jax.ShapeDtypeStruct((total, LANES), jnp.float32),
        compiler_params=pltpu.CompilerParams(vmem_limit_bytes=4 * 2**20),
    )(*(pltpu.with_memory_space_constraint(a, pltpu.HBM) for a in (*weights, *scales)))
    pieces = lax.all_gather(packed.astype(jnp.float16), "fs")
    blocks = pieces.shape[1] // rows
    terms = [pieces[:, blocks * rows + k].astype(jnp.float32) for k in range(3)]
    top = terms[0] + (terms[1] + terms[2]) * (1.0 / LOW)
    columns, start = [], 0
    for s in scales:
        columns.append(top[:, start : start + s.size].reshape(-1) * (1.0 / LIFT))
        start += s.size
    each = blocks // PARTS * rows
    parts = [
        pieces[:, k * each : (k + 1) * each].astype(jnp.float32).astype(jnp.bfloat16)
        for k in range(PARTS)
    ]
    return lax.optimization_barrier(parts), (jnp.concatenate(columns[:-1]), columns[-1])


def summed_rows(left, weight, scale):
    count = lax.axis_size("tp")
    chips = count // 2
    me = lax.axis_index("tp")
    chip, core = me // 2, me % 2
    rows = left.shape[0] // count

    def part(which, steps):
        blocks = []
        for step in steps:
            target = 2 * lax.rem(chip + (1 - 2 * which) * step + chips, chips) + which
            blocks.append(lax.dynamic_slice_in_dim(left, target * rows, rows, 0))
        these = blocks[0] if len(blocks) == 1 else jnp.concatenate(blocks, axis=0)
        total = lax.dot_general(
            these, weight, (((1,), (1,)), ((), ())), preferred_element_type=jnp.float32
        )
        return (total * scale).astype(jnp.bfloat16)

    def toward(sign):
        return [(i, (i + sign * (2 - 4 * (i % 2))) % count) for i in range(count)]

    def add(a, b):
        return a.astype(jnp.float32) + b.astype(jnp.float32)

    swap = [(i, i ^ 1) for i in range(count)]
    theirs = lax.ppermute(part(1 - core, (2,)), "tp", swap)
    far = add(part(core, (2,)), theirs).astype(jnp.bfloat16)
    others = part(1 - core, (0, 1, 3))
    far, others = lax.optimization_barrier((far, others))
    carried = lax.ppermute(far, "tp", toward(1))
    theirs = lax.ppermute(others, "tp", swap)
    pair = add(part(core, (0, 1, 3)), theirs)
    own, near, back = [pair[k * rows : (k + 1) * rows] for k in range(3)]
    behind = lax.ppermute(back.astype(jnp.bfloat16), "tp", toward(-1))
    onward = (near + carried.astype(jnp.float32)).astype(jnp.bfloat16)
    ahead = lax.ppermute(onward, "tp", toward(1))
    return (own + behind.astype(jnp.float32) + ahead.astype(jnp.float32)).astype(jnp.bfloat16)


def gate_kernel(tokens, gain, columns, taps, *refs):
    *pieces, out, mixer, weight, carry = refs

    @pl.when(pl.program_id(0) == 0)
    def _():
        carry[...] = jnp.zeros_like(carry)
        depth = weight.shape[0]
        rows = depth // pieces[0].shape[0]
        each = pieces[0].shape[1] // rows
        inputs = weight.shape[1] // LANES
        for k in range(inputs + mixer.shape[1] // LANES):
            low = k % each * rows
            full = pieces[k // each][:, low : low + rows, :]
            to, at = (weight, k) if k < inputs else (mixer, k - inputs)
            to[:, at * LANES : (at + 1) * LANES] = full.reshape(depth, LANES)

    values = tokens[...].astype(jnp.float32)
    inverse = lax.rsqrt(jnp.mean(values * values, axis=-1, keepdims=True) + EPS)
    normal = (values * inverse * gain[...]).astype(jnp.bfloat16)
    width = out.shape[1]

    def projected(at):
        cols = slice(at * width, (at + 1) * width)
        total = jnp.dot(normal, weight[:, cols], preferred_element_type=jnp.float32)
        return (total * columns[:, cols]).astype(jnp.bfloat16).astype(jnp.float32)

    product = projected(1) * projected(2)
    last = carry[...]
    carry[...] = product[-8:]
    row = lax.broadcasted_iota(jnp.int32, (8, width), 0)

    def shifted(by):
        moved = pltpu.roll(product, by, 0)
        head = jnp.where(row < by, pltpu.roll(last, by, 0), moved[:8])
        return jnp.concatenate([head, moved[8:]], axis=0)

    filtered = taps[0:1] * shifted(2) + taps[1:2] * shifted(1) + taps[2:3] * product
    out[...] = (projected(0) * filtered).astype(jnp.bfloat16)


def gated_rows(tokens, gain, pieces, columns, taps):
    rows, depth = tokens.shape
    width = taps.shape[1]
    whole = pl.BlockSpec(memory_space=pltpu.VMEM)
    return pl.pallas_call(
        gate_kernel,
        grid=(rows // ROWS,),
        in_specs=[pl.BlockSpec((ROWS, depth), lambda i: (i, 0))] + [whole] * (3 + len(pieces)),
        out_specs=[pl.BlockSpec((ROWS, width), lambda i: (i, 0)), whole],
        out_shape=[
            jax.ShapeDtypeStruct((rows, width), jnp.bfloat16),
            jax.ShapeDtypeStruct((depth, width), jnp.bfloat16),
        ],
        scratch_shapes=[
            pltpu.VMEM((depth, 3 * width), jnp.bfloat16),
            pltpu.VMEM((8, width), jnp.float32),
        ],
        compiler_params=pltpu.CompilerParams(
            dimension_semantics=("arbitrary",), vmem_limit_bytes=VMEM_BYTES
        ),
    )(pltpu.with_memory_space_constraint(tokens, pltpu.HBM), gain.reshape(1, -1), columns.reshape(1, -1), taps, *pieces)


def per_device(
    tokens,
    mixer_gain,
    outer_weight,
    inner_weight,
    value_weight,
    filter_taps,
    mixer_weight,
    outer_scale,
    inner_scale,
    value_scale,
    mixer_scale,
):
    pieces, columns = gathered(
        (outer_weight, inner_weight, value_weight, mixer_weight.T),
        (outer_scale, inner_scale, value_scale, mixer_scale),
    )
    gated, mixer_full = gated_rows(tokens, mixer_gain, pieces, columns[0], filter_taps)
    return summed_rows(gated, mixer_full, columns[1])


def solution(mesh):
    in_specs = (
        P(("grp", "fs"), None),
        P(),
        P("fs", "tp"),
        P("fs", "tp"),
        P("fs", "tp"),
        P(None, "tp"),
        P("tp", "fs"),
        P("tp", "fs"),
        P("tp", "fs"),
        P("tp", "fs"),
        P(None, "fs"),
    )
    out_specs = P(("grp", "fs", "tp"), None)
    return jax.shard_map(
        per_device, mesh=mesh, in_specs=in_specs, out_specs=out_specs, check_vma=False
    )
```

```python
import jax
import jax.numpy as jnp
from jax import lax
from jax.experimental import pallas as pl
from jax.experimental.pallas import tpu as pltpu
from jax.sharding import PartitionSpec as P


EPS = 1e-06
LIFT = 2.0**18
LOW = 2.0**12
LANES = 128
PARTS = 2
ROWS = 256
VMEM_BYTES = 28 * 2**20


def pack_kernel(*refs):
    *arrays, out = refs
    weights, scales = arrays[:4], arrays[4:]
    at = 0
    for w in weights:
        rows, width = w.shape
        for k in range(0, width, LANES):
            block = w[:, k : k + LANES].astype(jnp.bfloat16).astype(jnp.float32)
            out[at : at + rows, :] = block * LIFT
            at += rows
    out[at:, :] = jnp.zeros((out.shape[0] - at, LANES), jnp.float32)
    start = 0
    for s in scales:
        value, stop = s[...], start + s.shape[1]
        high = value.astype(jnp.bfloat16).astype(jnp.float32)
        rest = (value - high) * LOW
        middle = rest.astype(jnp.bfloat16).astype(jnp.float32)
        for k, term in enumerate((high, middle, rest - middle)):
            out[at + k : at + k + 1, start:stop] = term
        start = stop


def gathered(weights, scales):
    rows = weights[0].shape[0]
    total = sum(w.shape[1] for w in weights) // LANES * rows + 8
    packed = pl.pallas_call(
        pack_kernel,
        out_shape=jax.ShapeDtypeStruct((total, LANES), jnp.float32),
        compiler_params=pltpu.CompilerParams(vmem_limit_bytes=4 * 2**20),
    )(*(pltpu.with_memory_space_constraint(a, pltpu.HBM) for a in (*weights, *scales)))
    pieces = lax.all_gather(packed.astype(jnp.float16), "fs")
    blocks = pieces.shape[1] // rows
    terms = [pieces[:, blocks * rows + k].astype(jnp.float32) for k in range(3)]
    top = terms[0] + (terms[1] + terms[2]) * (1.0 / LOW)
    columns, start = [], 0
    for s in scales:
        columns.append(top[:, start : start + s.size].reshape(-1) * (1.0 / LIFT))
        start += s.size
    each = blocks // PARTS * rows
    parts = [
        pieces[:, k * each : (k + 1) * each].astype(jnp.float32).astype(jnp.bfloat16)
        for k in range(PARTS)
    ]
    return lax.optimization_barrier(parts), (jnp.concatenate(columns[:-1]), columns[-1])


def summed_rows(left, weight, scale):
    count = lax.axis_size("tp")
    chips = count // 2
    me = lax.axis_index("tp")
    chip, core = me // 2, me % 2
    rows = left.shape[0] // count

    def part(which, steps):
        blocks = []
        for step in steps:
            target = 2 * lax.rem(chip + (1 - 2 * which) * step + chips, chips) + which
            blocks.append(lax.dynamic_slice_in_dim(left, target * rows, rows, 0))
        these = blocks[0] if len(blocks) == 1 else jnp.concatenate(blocks, axis=0)
        total = lax.dot_general(
            these, weight, (((1,), (1,)), ((), ())), preferred_element_type=jnp.float32
        )
        return (total * scale).astype(jnp.bfloat16)

    def toward(sign):
        return [(i, (i + sign * (2 - 4 * (i % 2))) % count) for i in range(count)]

    def add(a, b):
        return a.astype(jnp.float32) + b.astype(jnp.float32)

    swap = [(i, i ^ 1) for i in range(count)]
    theirs = lax.ppermute(part(1 - core, (2, 3)), "tp", swap)
    outward = add(part(core, (2, 3)), theirs).astype(jnp.bfloat16)
    others = part(1 - core, (0, 1))
    outward, others = lax.optimization_barrier((outward, others))
    carried = lax.ppermute(outward[:rows], "tp", toward(1))
    behind = lax.ppermute(outward[rows:], "tp", toward(-1))
    theirs = lax.ppermute(others, "tp", swap)
    pair = add(part(core, (0, 1)), theirs)
    own = pair[:rows].astype(jnp.bfloat16)
    onward = (pair[rows:] + carried.astype(jnp.float32)).astype(jnp.bfloat16)
    ahead = lax.ppermute(onward, "tp", toward(1))
    return (add(own, behind) + ahead.astype(jnp.float32)).astype(jnp.bfloat16)


def gate_kernel(tokens, gain, columns, taps, *refs):
    *pieces, out, mixer, weight, carry = refs

    @pl.when(pl.program_id(0) == 0)
    def _():
        carry[...] = jnp.zeros_like(carry)
        depth = weight.shape[0]
        rows = depth // pieces[0].shape[0]
        each = pieces[0].shape[1] // rows
        inputs = weight.shape[1] // LANES
        for k in range(inputs + mixer.shape[1] // LANES):
            low = k % each * rows
            full = pieces[k // each][:, low : low + rows, :]
            to, at = (weight, k) if k < inputs else (mixer, k - inputs)
            to[:, at * LANES : (at + 1) * LANES] = full.reshape(depth, LANES)

    values = tokens[...].astype(jnp.float32)
    inverse = lax.rsqrt(jnp.mean(values * values, axis=-1, keepdims=True) + EPS)
    normal = (values * inverse * gain[...]).astype(jnp.bfloat16)
    width = out.shape[1]

    def projected(at):
        cols = slice(at * width, (at + 1) * width)
        total = jnp.dot(normal, weight[:, cols], preferred_element_type=jnp.float32)
        return (total * columns[:, cols]).astype(jnp.bfloat16).astype(jnp.float32)

    product = projected(1) * projected(2)
    last = carry[...]
    carry[...] = product[-8:]
    row = lax.broadcasted_iota(jnp.int32, (8, width), 0)

    def shifted(by):
        moved = pltpu.roll(product, by, 0)
        head = jnp.where(row < by, pltpu.roll(last, by, 0), moved[:8])
        return jnp.concatenate([head, moved[8:]], axis=0)

    filtered = taps[0:1] * shifted(2) + taps[1:2] * shifted(1) + taps[2:3] * product
    out[...] = (projected(0) * filtered).astype(jnp.bfloat16)


def gated_rows(tokens, gain, pieces, columns, taps):
    rows, depth = tokens.shape
    width = taps.shape[1]
    whole = pl.BlockSpec(memory_space=pltpu.VMEM)
    return pl.pallas_call(
        gate_kernel,
        grid=(rows // ROWS,),
        in_specs=[pl.BlockSpec((ROWS, depth), lambda i: (i, 0))] + [whole] * (3 + len(pieces)),
        out_specs=[pl.BlockSpec((ROWS, width), lambda i: (i, 0)), whole],
        out_shape=[
            jax.ShapeDtypeStruct((rows, width), jnp.bfloat16),
            jax.ShapeDtypeStruct((depth, width), jnp.bfloat16),
        ],
        scratch_shapes=[
            pltpu.VMEM((depth, 3 * width), jnp.bfloat16),
            pltpu.VMEM((8, width), jnp.float32),
        ],
        compiler_params=pltpu.CompilerParams(
            dimension_semantics=("arbitrary",), vmem_limit_bytes=VMEM_BYTES
        ),
    )(pltpu.with_memory_space_constraint(tokens, pltpu.HBM), gain.reshape(1, -1), columns.reshape(1, -1), taps, *pieces)


def per_device(
    tokens,
    mixer_gain,
    outer_weight,
    inner_weight,
    value_weight,
    filter_taps,
    mixer_weight,
    outer_scale,
    inner_scale,
    value_scale,
    mixer_scale,
):
    pieces, columns = gathered(
        (outer_weight, inner_weight, value_weight, mixer_weight.T),
        (outer_scale, inner_scale, value_scale, mixer_scale),
    )
    gated, mixer_full = gated_rows(tokens, mixer_gain, pieces, columns[0], filter_taps)
    return summed_rows(gated, mixer_full, columns[1])


def solution(mesh):
    in_specs = (
        P(("grp", "fs"), None),
        P(),
        P("fs", "tp"),
        P("fs", "tp"),
        P("fs", "tp"),
        P(None, "tp"),
        P("tp", "fs"),
        P("tp", "fs"),
        P("tp", "fs"),
        P("tp", "fs"),
        P(None, "fs"),
    )
    out_specs = P(("grp", "fs", "tp"), None)
    return jax.shard_map(
        per_device, mesh=mesh, in_specs=in_specs, out_specs=out_specs, check_vma=False
    )
```

```python
import jax
import jax.numpy as jnp
from jax import lax
from jax.experimental import pallas as pl
from jax.experimental.pallas import tpu as pltpu
from jax.sharding import PartitionSpec as P


EPS = 1e-06
LIFT = 2.0**18
LOW = 2.0**12
LANES = 128
PARTS = 2
ROWS = 512
SUB = 128
VMEM_BYTES = 32 * 2**20


def pack_kernel(*refs):
    *arrays, out = refs
    weights, scales = arrays[:4], arrays[4:]
    at = 0
    for w in weights:
        rows, width = w.shape
        for k in range(0, width, LANES):
            block = w[:, k : k + LANES].astype(jnp.bfloat16).astype(jnp.float32)
            out[at : at + rows, :] = block * LIFT
            at += rows
    out[at:, :] = jnp.zeros((out.shape[0] - at, LANES), jnp.float32)
    start = 0
    for s in scales:
        value, stop = s[...], start + s.shape[1]
        high = value.astype(jnp.bfloat16).astype(jnp.float32)
        rest = (value - high) * LOW
        middle = rest.astype(jnp.bfloat16).astype(jnp.float32)
        for k, term in enumerate((high, middle, rest - middle)):
            out[at + k : at + k + 1, start:stop] = term
        start = stop


def gathered(weights, scales):
    rows = weights[0].shape[0]
    total = sum(w.shape[1] for w in weights) // LANES * rows + 8
    packed = pl.pallas_call(
        pack_kernel,
        out_shape=jax.ShapeDtypeStruct((total, LANES), jnp.float32),
        compiler_params=pltpu.CompilerParams(vmem_limit_bytes=4 * 2**20),
    )(*(pltpu.with_memory_space_constraint(a, pltpu.HBM) for a in (*weights, *scales)))
    pieces = lax.all_gather(packed.astype(jnp.float16), "fs")
    blocks = pieces.shape[1] // rows
    terms = [pieces[:, blocks * rows + k].astype(jnp.float32) for k in range(3)]
    top = terms[0] + (terms[1] + terms[2]) * (1.0 / LOW)
    columns, start = [], 0
    for s in scales:
        columns.append(top[:, start : start + s.size].reshape(-1) * (1.0 / LIFT))
        start += s.size
    each = blocks // PARTS * rows
    parts = [
        pieces[:, k * each : (k + 1) * each].astype(jnp.float32).astype(jnp.bfloat16)
        for k in range(PARTS)
    ]
    return lax.optimization_barrier(parts), (jnp.concatenate(columns[:-1]), columns[-1])


def summed_rows(left, weight, scale):
    count = lax.axis_size("tp")
    chips = count // 2
    me = lax.axis_index("tp")
    chip, core = me // 2, me % 2
    rows = left.shape[0] // count

    def part(which, steps):
        blocks = []
        for step in steps:
            target = 2 * lax.rem(chip + (1 - 2 * which) * step + chips, chips) + which
            blocks.append(lax.dynamic_slice_in_dim(left, target * rows, rows, 0))
        these = blocks[0] if len(blocks) == 1 else jnp.concatenate(blocks, axis=0)
        total = lax.dot_general(
            these, weight, (((1,), (1,)), ((), ())), preferred_element_type=jnp.float32
        )
        return (total * scale).astype(jnp.bfloat16)

    def toward(sign):
        return [(i, (i + sign * (2 - 4 * (i % 2))) % count) for i in range(count)]

    def add(a, b):
        return a.astype(jnp.float32) + b.astype(jnp.float32)

    swap = [(i, i ^ 1) for i in range(count)]
    theirs = lax.ppermute(part(1 - core, (2, 3)), "tp", swap)
    outward = add(part(core, (2, 3)), theirs).astype(jnp.bfloat16)
    others = part(1 - core, (0, 1))
    outward, others = lax.optimization_barrier((outward, others))
    carried = lax.ppermute(outward[:rows], "tp", toward(1))
    behind = lax.ppermute(outward[rows:], "tp", toward(-1))
    theirs = lax.ppermute(others, "tp", swap)
    pair = add(part(core, (0, 1)), theirs)
    own = pair[:rows].astype(jnp.bfloat16)
    onward = (pair[rows:] + carried.astype(jnp.float32)).astype(jnp.bfloat16)
    ahead = lax.ppermute(onward, "tp", toward(1))
    return (add(own, behind) + ahead.astype(jnp.float32)).astype(jnp.bfloat16)


def gate_kernel(tokens, gain, columns, taps, *refs):
    *pieces, far_piece, out, mixer, weight, carry, near_piece, ready = refs
    width = out.shape[1]

    @pl.when(pl.program_id(0) == 0)
    def _():
        fetch = pltpu.make_async_copy(far_piece, near_piece, ready)
        fetch.start()
        carry[...] = jnp.zeros_like(carry)
        depth = weight.shape[0]
        rows = depth // near_piece.shape[0]
        inputs, at = weight.shape[1] // LANES, 0
        for piece in (*pieces, near_piece):
            if piece is near_piece:
                fetch.wait()
            for low in range(0, piece.shape[1], rows):
                full = piece[:, low : low + rows, :].reshape(depth, LANES)
                to, k = (weight, at) if at < inputs else (mixer, at - inputs)
                to[:, k * LANES : (k + 1) * LANES] = full
                at += 1

    last = carry[...]
    row = lax.broadcasted_iota(jnp.int32, (8, width), 0)
    for low in range(0, ROWS, SUB):
        values = tokens[low : low + SUB, :].astype(jnp.float32)
        inverse = lax.rsqrt(jnp.mean(values * values, axis=-1, keepdims=True) + EPS)
        normal = (values * inverse * gain[...]).astype(jnp.bfloat16)

        def projected(at):
            cols = slice(at * width, (at + 1) * width)
            total = jnp.dot(normal, weight[:, cols], preferred_element_type=jnp.float32)
            return (total * columns[:, cols]).astype(jnp.bfloat16).astype(jnp.float32)

        product = projected(1) * projected(2)

        def shifted(by):
            moved = pltpu.roll(product, by, 0)
            head = jnp.where(row < by, pltpu.roll(last, by, 0), moved[:8])
            return jnp.concatenate([head, moved[8:]], axis=0)

        filtered = taps[0:1] * shifted(2) + taps[1:2] * shifted(1) + taps[2:3] * product
        out[low : low + SUB, :] = (projected(0) * filtered).astype(jnp.bfloat16)
        last = product[-8:]
    carry[...] = last


def gated_rows(tokens, gain, pieces, columns, taps):
    rows, depth = tokens.shape
    width = taps.shape[1]
    whole = pl.BlockSpec(memory_space=pltpu.VMEM)
    hbm = pl.BlockSpec(memory_space=pltpu.HBM)
    *pieces, far_piece = pieces
    return pl.pallas_call(
        gate_kernel,
        grid=(rows // ROWS,),
        in_specs=[pl.BlockSpec((ROWS, depth), lambda i: (i, 0))]
        + [whole] * (3 + len(pieces))
        + [hbm],
        out_specs=[pl.BlockSpec((ROWS, width), lambda i: (i, 0)), whole],
        out_shape=[
            jax.ShapeDtypeStruct((rows, width), jnp.bfloat16),
            jax.ShapeDtypeStruct((depth, width), jnp.bfloat16),
        ],
        scratch_shapes=[
            pltpu.VMEM((depth, 3 * width), jnp.bfloat16),
            pltpu.VMEM((8, width), jnp.float32),
            pltpu.VMEM(far_piece.shape, far_piece.dtype),
            pltpu.SemaphoreType.DMA,
        ],
        compiler_params=pltpu.CompilerParams(
            dimension_semantics=("arbitrary",), vmem_limit_bytes=VMEM_BYTES
        ),
    )(
        pltpu.with_memory_space_constraint(tokens, pltpu.HBM),
        gain.reshape(1, -1),
        columns.reshape(1, -1),
        taps,
        *pieces,
        pltpu.with_memory_space_constraint(far_piece, pltpu.HBM),
    )


def per_device(
    tokens,
    mixer_gain,
    outer_weight,
    inner_weight,
    value_weight,
    filter_taps,
    mixer_weight,
    outer_scale,
    inner_scale,
    value_scale,
    mixer_scale,
):
    pieces, columns = gathered(
        (outer_weight, inner_weight, value_weight, mixer_weight.T),
        (outer_scale, inner_scale, value_scale, mixer_scale),
    )
    gated, mixer_full = gated_rows(tokens, mixer_gain, pieces, columns[0], filter_taps)
    return summed_rows(gated, mixer_full, columns[1])


def solution(mesh):
    in_specs = (
        P(("grp", "fs"), None),
        P(),
        P("fs", "tp"),
        P("fs", "tp"),
        P("fs", "tp"),
        P(None, "tp"),
        P("tp", "fs"),
        P("tp", "fs"),
        P("tp", "fs"),
        P("tp", "fs"),
        P(None, "fs"),
    )
    out_specs = P(("grp", "fs", "tp"), None)
    return jax.shard_map(
        per_device, mesh=mesh, in_specs=in_specs, out_specs=out_specs, check_vma=False
    )
```

```python
import jax
import jax.numpy as jnp
from jax import lax
from jax.experimental import pallas as pl
from jax.experimental.pallas import tpu as pltpu
from jax.sharding import PartitionSpec as P


EPS = 1e-06
LIFT = 2.0**18
LOW = 2.0**12
LANES = 128
PARTS = 4
ROWS = 512
SUB = 128
VMEM_BYTES = 32 * 2**20


def pack_kernel(*refs):
    *arrays, out = refs
    weights, scales = arrays[:4], arrays[4:]
    at = 0
    for w in weights:
        rows, width = w.shape
        for k in range(0, width, LANES):
            block = w[:, k : k + LANES].astype(jnp.bfloat16).astype(jnp.float32)
            out[at : at + rows, :] = block * LIFT
            at += rows
    out[at:, :] = jnp.zeros((out.shape[0] - at, LANES), jnp.float32)
    start = 0
    for s in scales:
        value, stop = s[...], start + s.shape[1]
        high = value.astype(jnp.bfloat16).astype(jnp.float32)
        rest = (value - high) * LOW
        middle = rest.astype(jnp.bfloat16).astype(jnp.float32)
        for k, term in enumerate((high, middle, rest - middle)):
            out[at + k : at + k + 1, start:stop] = term
        start = stop


def gathered(weights, scales):
    rows = weights[0].shape[0]
    total = sum(w.shape[1] for w in weights) // LANES * rows + 8
    packed = pl.pallas_call(
        pack_kernel,
        out_shape=jax.ShapeDtypeStruct((total, LANES), jnp.float32),
        compiler_params=pltpu.CompilerParams(vmem_limit_bytes=4 * 2**20),
    )(*(pltpu.with_memory_space_constraint(a, pltpu.HBM) for a in (*weights, *scales)))
    pieces = lax.all_gather(packed.astype(jnp.float16), "fs")
    blocks = pieces.shape[1] // rows
    terms = [pieces[:, blocks * rows + k].astype(jnp.float32) for k in range(3)]
    top = terms[0] + (terms[1] + terms[2]) * (1.0 / LOW)
    columns, start = [], 0
    for s in scales:
        columns.append(top[:, start : start + s.size].reshape(-1) * (1.0 / LIFT))
        start += s.size
    each = blocks // PARTS * rows
    parts = [
        pieces[:, k * each : (k + 1) * each].astype(jnp.float32).astype(jnp.bfloat16)
        for k in range(PARTS)
    ]
    return lax.optimization_barrier(parts), (jnp.concatenate(columns[:-1]), columns[-1])


def summed_rows(left, weight, scale):
    count = lax.axis_size("tp")
    chips = count // 2
    me = lax.axis_index("tp")
    chip, core = me // 2, me % 2
    rows = left.shape[0] // count

    def part(which, steps):
        blocks = []
        for step in steps:
            target = 2 * lax.rem(chip + (1 - 2 * which) * step + chips, chips) + which
            blocks.append(lax.dynamic_slice_in_dim(left, target * rows, rows, 0))
        these = blocks[0] if len(blocks) == 1 else jnp.concatenate(blocks, axis=0)
        total = lax.dot_general(
            these, weight, (((1,), (1,)), ((), ())), preferred_element_type=jnp.float32
        )
        return (total * scale).astype(jnp.bfloat16)

    def toward(sign):
        return [(i, (i + sign * (2 - 4 * (i % 2))) % count) for i in range(count)]

    def add(a, b):
        return a.astype(jnp.float32) + b.astype(jnp.float32)

    swap = [(i, i ^ 1) for i in range(count)]
    theirs = lax.ppermute(part(1 - core, (2, 3)), "tp", swap)
    outward = add(part(core, (2, 3)), theirs).astype(jnp.bfloat16)
    others = part(1 - core, (0, 1))
    outward, others = lax.optimization_barrier((outward, others))
    carried = lax.ppermute(outward[:rows], "tp", toward(1))
    behind = lax.ppermute(outward[rows:], "tp", toward(-1))
    theirs = lax.ppermute(others, "tp", swap)
    pair = add(part(core, (0, 1)), theirs)
    own = pair[:rows].astype(jnp.bfloat16)
    onward = (pair[rows:] + carried.astype(jnp.float32)).astype(jnp.bfloat16)
    ahead = lax.ppermute(onward, "tp", toward(1))
    return (add(own, behind) + ahead.astype(jnp.float32)).astype(jnp.bfloat16)


def gate_kernel(tokens, gain, columns, taps, *refs):
    *pieces, far_piece, out, mixer, weight, carry, near_piece, ready = refs
    width = out.shape[1]

    @pl.when(pl.program_id(0) == 0)
    def _():
        pltpu.make_async_copy(far_piece, near_piece, ready).start()
        carry[...] = jnp.zeros_like(carry)
        depth = weight.shape[0]
        rows = depth // near_piece.shape[0]
        at = 0
        for piece in pieces:
            for low in range(0, piece.shape[1], rows):
                full = piece[:, low : low + rows, :].reshape(depth, LANES)
                weight[:, at * LANES : (at + 1) * LANES] = full
                at += 1

    @pl.when(pl.program_id(0) == pl.num_programs(0) - 1)
    def _():
        pltpu.make_async_copy(far_piece, near_piece, ready).wait()
        depth = mixer.shape[0]
        rows = depth // near_piece.shape[0]
        for at in range(mixer.shape[1] // LANES):
            full = near_piece[:, at * rows : (at + 1) * rows, :].reshape(depth, LANES)
            mixer[:, at * LANES : (at + 1) * LANES] = full

    last = carry[...]
    row = lax.broadcasted_iota(jnp.int32, (8, width), 0)
    for low in range(0, ROWS, SUB):
        values = tokens[low : low + SUB, :].astype(jnp.float32)
        inverse = lax.rsqrt(jnp.mean(values * values, axis=-1, keepdims=True) + EPS)
        normal = (values * inverse * gain[...]).astype(jnp.bfloat16)

        def projected(at):
            cols = slice(at * width, (at + 1) * width)
            total = jnp.dot(normal, weight[:, cols], preferred_element_type=jnp.float32)
            return (total * columns[:, cols]).astype(jnp.bfloat16).astype(jnp.float32)

        product = projected(1) * projected(2)

        def shifted(by):
            moved = pltpu.roll(product, by, 0)
            head = jnp.where(row < by, pltpu.roll(last, by, 0), moved[:8])
            return jnp.concatenate([head, moved[8:]], axis=0)

        filtered = taps[0:1] * shifted(2) + taps[1:2] * shifted(1) + taps[2:3] * product
        out[low : low + SUB, :] = (projected(0) * filtered).astype(jnp.bfloat16)
        last = product[-8:]
    carry[...] = last


def gated_rows(tokens, gain, pieces, columns, taps):
    rows, depth = tokens.shape
    width = taps.shape[1]
    whole = pl.BlockSpec(memory_space=pltpu.VMEM)
    hbm = pl.BlockSpec(memory_space=pltpu.HBM)
    *pieces, far_piece = pieces
    return pl.pallas_call(
        gate_kernel,
        grid=(rows // ROWS,),
        in_specs=[pl.BlockSpec((ROWS, depth), lambda i: (i, 0))]
        + [whole] * (3 + len(pieces))
        + [hbm],
        out_specs=[pl.BlockSpec((ROWS, width), lambda i: (i, 0)), whole],
        out_shape=[
            jax.ShapeDtypeStruct((rows, width), jnp.bfloat16),
            jax.ShapeDtypeStruct((depth, width), jnp.bfloat16),
        ],
        scratch_shapes=[
            pltpu.VMEM((depth, 3 * width), jnp.bfloat16),
            pltpu.VMEM((8, width), jnp.float32),
            pltpu.VMEM(far_piece.shape, far_piece.dtype),
            pltpu.SemaphoreType.DMA,
        ],
        compiler_params=pltpu.CompilerParams(
            dimension_semantics=("arbitrary",), vmem_limit_bytes=VMEM_BYTES
        ),
    )(
        pltpu.with_memory_space_constraint(tokens, pltpu.HBM),
        gain.reshape(1, -1),
        columns.reshape(1, -1),
        taps,
        *pieces,
        pltpu.with_memory_space_constraint(far_piece, pltpu.HBM),
    )


def per_device(
    tokens,
    mixer_gain,
    outer_weight,
    inner_weight,
    value_weight,
    filter_taps,
    mixer_weight,
    outer_scale,
    inner_scale,
    value_scale,
    mixer_scale,
):
    pieces, columns = gathered(
        (outer_weight, inner_weight, value_weight, mixer_weight.T),
        (outer_scale, inner_scale, value_scale, mixer_scale),
    )
    gated, mixer_full = gated_rows(tokens, mixer_gain, pieces, columns[0], filter_taps)
    return summed_rows(gated, mixer_full, columns[1])


def solution(mesh):
    in_specs = (
        P(("grp", "fs"), None),
        P(),
        P("fs", "tp"),
        P("fs", "tp"),
        P("fs", "tp"),
        P(None, "tp"),
        P("tp", "fs"),
        P("tp", "fs"),
        P("tp", "fs"),
        P("tp", "fs"),
        P(None, "fs"),
    )
    out_specs = P(("grp", "fs", "tp"), None)
    return jax.shard_map(
        per_device, mesh=mesh, in_specs=in_specs, out_specs=out_specs, check_vma=False
    )
```
